32 devices in a mesh: ep: 8 (over z, core), tp: 4 (over y, x).
Axes of the slice: x: 2, y: 2, z: 4, core: 2. Of those that a mesh axis runs over, the one named last changes fastest.
Arguments:
- query_rows: bfloat16 [4096, 2048], P('ep', 'tp'), may hold values from -6 to 6
- key_rows: bfloat16 [4096, 2048], P('ep', 'tp'), may hold values from -6 to 6
- value_rows: bfloat16 [4096, 4096], P('ep', 'tp'), may hold values from -6 to 6
- in_gate: float32 [16, 4096], P('tp', 'ep'), may hold values from -120 to 120
- forget_gate: float32 [16, 4096], P('tp', 'ep'), may hold values from -2 to 20
- out_gate: bfloat16 [4096, 4096], P('ep', 'tp'), may hold values from -6 to 6
- head_gain: float32 [4096], P('tp'), may hold values from 0.1 to 1.9
- mix_weight: bfloat16 [4096, 4096], P(None, 'tp'), may hold values from -0.09375 to 0.09375
- expert_input: bfloat16 [2048, 4096], P('ep', 'tp'), may hold values from -30 to 30
- routes: int32 [2048, 2], P('ep'), may hold values from 0 to 7, all different within a row; in each aligned block of 256 rows (0 to 255, 256 to 511, ...) at most 128 rows name the same one
- route_weight: float32 [2048, 2], P('ep'), may hold values from 0.25 to 1.25
- gate_weight: bfloat16 [8, 1024, 4096], P('ep', 'tp'), may hold values from -0.09375 to 0.09375
- up_weight: bfloat16 [8, 1024, 4096], P('ep', 'tp'), may hold values from -0.09375 to 0.09375
- down_weight: bfloat16 [8, 1024, 4096], P('ep', None, 'tp'), may hold values from -0.1875 to 0.1875
Outputs:
- mixer_out: bfloat16 [4096, 4096], P('ep', 'tp')
- expert_out: bfloat16 [2048, 4096], P('ep', 'tp')
The draws below stay inside these ranges and needn't reach their ends.
Inputs may be any that keep to these rules, and one draw needn't show every extreme that they name: `routes`: each row names 2 different experts. In the rows of one device no expert is named by more than 128 rows, and in the rows of some device an expert is named by exactly 128 rows.
All inputs are finite; a program needn't handle non-finite values.
Results may differ from the reference program's by a relative error of at most 0.0057.
Values may be sent and summed in bfloat16 or wider, within the bound.
A program may use at most 128 MiB of HBM per device.

```python
import math
import jax
import jax.numpy as jnp
import numpy as np
from jax import lax

D = 4096
HEADS = 16
QK = 128
FF = 1024
TOP = 2
BLOCK = 64
ROWS_A = 512
ROWS_B = 256
TOKENS_A = 4096
TOKENS_B = 2048
EXPERTS = 8
CAP = 128
N_EP = 8


def draw_in_gate(key, part):
    base = jnp.clip(jax.random.normal(jax.random.fold_in(key, 11), (HEADS, TOKENS_A), jnp.float32), -4.0, 4.0)
    return base


def draw_forget_gate(key, part):
    slow_share = 0.5
    slow_heads = jax.random.bernoulli(jax.random.fold_in(key, 21), slow_share, (HEADS, 1))
    level = jnp.where(slow_heads, math.log(TOKENS_A) + 0.5, 3.5)
    span_total = TOKENS_A // ROWS_A
    drift = jax.random.uniform(jax.random.fold_in(key, 22), (HEADS, span_total), jnp.float32, -1.0, 1.0)
    noise = 0.7 * jnp.clip(jax.random.normal(jax.random.fold_in(key, 23), (HEADS, TOKENS_A), jnp.float32), -4.0, 4.0)
    return level + jnp.repeat(drift, ROWS_A, axis=1) + noise


def draw_expert_input(key, part):
    row_scale = jnp.exp(jax.random.uniform(jax.random.fold_in(key, 31), (TOKENS_B, 1), jnp.float32, -0.7, 0.7))
    base = jnp.clip(jax.random.normal(jax.random.fold_in(key, 34), (TOKENS_B, D), jnp.float32), -4.0, 4.0)
    return (base * row_scale).astype(jnp.bfloat16)


def steps_of(rng, extent, split, low, high):
    loudness, own = 1.0, jax.random.fold_in(rng, 6)
    for axis_at, shards_of in split:
        steps = jnp.exp(jax.random.uniform(jax.random.fold_in(own, axis_at), (shards_of,), jnp.float32, low / len(split), high / len(split)))
        loudness = loudness * jnp.repeat(steps, extent[axis_at] // shards_of).reshape([-1 if axis == axis_at else 1 for axis in range(len(extent))])
    return loudness


def deal_out(key, own, number, rows, count, top, bound, slope):
    order = jax.random.permutation(key, count)
    packed, usual = load_shares(count, rows * top, bound, slope, True), load_shares(count, rows * top, bound, slope, False)
    places = jnp.arange(count)

    def named(tallies, offset_by):
        used = int((tallies > 0).sum())
        fixed = max(1, used // 4)
        shifted = fixed + (places - fixed + offset_by * (used - fixed)) % max(1, count - fixed)
        return jnp.zeros((count,), jnp.int32).at[order[jnp.where(places < fixed, places, shifted)]].set(jnp.asarray(tallies, jnp.int32))

    tallies = jnp.where(number % 4 == 0, named(packed, number // 4), named(usual, number - number // 4 - 1))
    mixed = jax.random.permutation(jax.random.fold_in(own, 3), count)
    donor, taker = mixed[0:count // 2 * 2:2], mixed[1:count // 2 * 2:2]
    room = jnp.minimum(tallies[donor] - 1, bound - tallies[taker]) // 2
    room = jnp.where((donor == order[0]) | (taker == order[0]) | (tallies[taker] == 0), 0, jnp.maximum(room, 0))
    shifted = jax.random.randint(jax.random.fold_in(own, 4), (count // 2,), 0, 1 << 20) % (room + 1)
    tallies = tallies.at[donor].add(-shifted).at[taker].add(shifted)
    labels = jnp.searchsorted(jnp.cumsum(tallies), jnp.arange(rows * top), side="right").astype(jnp.int32)
    listing = labels.reshape(top, rows).T
    listing = listing[jax.random.permutation(jax.random.fold_in(own, 1), rows)]
    offset_by = jax.random.randint(jax.random.fold_in(own, 2), (rows, 1), 0, top)
    return jnp.take_along_axis(listing, (jnp.arange(top)[None, :] + offset_by) % top, axis=1)


def load_shares(amount, total, bound, lean, full):
    weights = [(1 << 20) // math.isqrt(grade ** lean) + 1 for grade in range(1, amount + 1)]
    largest = bound if full else min(bound, max(-(-total // amount), total * weights[0] // sum(weights)))
    least = 1 if total - largest >= amount - 1 else 0
    given, rest = [largest] + [least] * (amount - 1), total - largest - least * (amount - 1)
    while rest > 0:
        free = [i for i in range(1, amount) if given[i] < largest] or [i for i in range(1, amount) if given[i] < bound]
        mass, remaining = sum([weights[i] for i in free]), rest
        for i in free:
            extra = min(bound - given[i], max(1, remaining * weights[i] // mass), rest)
            given[i] = given[i] + extra
            rest = rest - extra
    return np.array(given)


def centred(key, dims, scale, bound, cuts=(), kind=jnp.bfloat16):
    level = steps_of(key, dims, cuts, -0.22, 0.18) if cuts else 1.0
    entries = jax.random.normal(key, dims, jnp.float32) * scale * level
    return jnp.minimum(jnp.maximum(entries, -bound), bound).astype(kind)


def setup_inputs(seed: int = 0) -> dict:
    key_of = jax.random.split(jax.random.key(seed), 15)
    query_rows = centred(key_of[0], (TOKENS_A, HEADS * QK), 1.0, 6.0, ((0, 8), (1, 4)))
    key_rows = centred(key_of[1], (TOKENS_A, HEADS * QK), 1.0, 6.0, ((0, 8), (1, 4)))
    value_rows = centred(key_of[2], (TOKENS_A, D), 1.0, 6.0, ((0, 8), (1, 4)))
    in_gate = draw_in_gate(jax.random.fold_in(key_of[14], 71), 0)
    forget_gate = draw_forget_gate(jax.random.fold_in(key_of[14], 71), 0)
    out_gate = centred(key_of[5], (TOKENS_A, D), 1.0, 6.0, ((0, 8), (1, 4)))
    head_gain = jnp.clip(1.0 + 0.18 * jax.random.normal(key_of[6], (D,), jnp.float32), 0.1, 1.9)
    mix_weight = centred(key_of[7], (D, D), D ** -0.5, 0.09375, ((1, 4),))
    expert_input = draw_expert_input(jax.random.fold_in(key_of[14], 71), 0)
    routes_keys = jax.random.split(jax.random.fold_in(key_of[9], 1), TOKENS_B // ROWS_B)
    routes_turns = jax.random.permutation(jax.random.fold_in(key_of[9], 3), TOKENS_B // ROWS_B)
    routes = jax.vmap(lambda own, number: deal_out(jax.random.fold_in(key_of[9], 2), own, number, ROWS_B, EXPERTS, TOP, CAP, 1))(routes_keys, routes_turns).reshape((TOKENS_B, TOP))
    route_weight = jnp.clip(0.25 + 1.0 * jax.random.uniform(key_of[10], (TOKENS_B, TOP), jnp.float32) ** steps_of(key_of[10], (TOKENS_B, TOP), ((0, 8),), -0.2, 0.2), 0.25, 1.25)
    gate_weight = centred(key_of[11], (EXPERTS, FF, D), D ** -0.5, 0.09375, ((0, 8), (1, 4)))
    up_weight = centred(key_of[12], (EXPERTS, FF, D), D ** -0.5, 0.09375, ((0, 8), (1, 4)))
    down_weight = centred(key_of[13], (EXPERTS, FF, D), FF ** -0.5, 0.1875, ((0, 8), (2, 4)))
    return dict(query_rows=query_rows, key_rows=key_rows, value_rows=value_rows, in_gate=in_gate, forget_gate=forget_gate, out_gate=out_gate, head_gain=head_gain, mix_weight=mix_weight, expert_input=expert_input, routes=routes, route_weight=route_weight, gate_weight=gate_weight, up_weight=up_weight, down_weight=down_weight)


EPSILON = 1e-06
LOG_FLOOR = -1e+30
HIGHEST_PRECISION = lax.Precision.HIGHEST

def combine(first_part, second_part):
    decay_first, max_first, memory_first, normal_first = first_part
    decay_second, max_second, memory_second, normal_second = second_part
    running_max = jnp.maximum(decay_second + max_first, max_second)
    keep_first = jnp.exp(decay_second + max_first - running_max)
    keep_second = jnp.exp(max_second - running_max)
    memory = keep_first[..., None, None] * memory_first + keep_second[..., None, None] * memory_second
    normalizer = keep_first[..., None] * normal_first + keep_second[..., None] * normal_second
    return (decay_first + decay_second, running_max, memory, normalizer)

def identity_state(head_count, key_width, value_width):
    return (jnp.zeros((head_count,), jnp.float32), jnp.full((head_count,), LOG_FLOOR, jnp.float32), jnp.zeros((head_count, key_width, value_width), jnp.float32), jnp.zeros((head_count, key_width), jnp.float32))

def halfprod(form, left, right):
    return jnp.einsum(form, left.astype(jnp.float32), right.astype(jnp.float32), precision=HIGHEST_PRECISION)

def prepare(query_heads, key_heads, value_heads, in_gate, forget_gate):
    head_count, length, key_width = query_heads.shape
    block_count = length // BLOCK
    query_blocks = query_heads.reshape(head_count, block_count, BLOCK, key_width)
    key_blocks = key_heads.reshape(head_count, block_count, BLOCK, key_width)
    value_blocks = value_heads.reshape(head_count, block_count, BLOCK, value_heads.shape[-1])
    log_input = in_gate.reshape(head_count, block_count, BLOCK)
    cumulative = jnp.cumsum(jax.nn.log_sigmoid(forget_gate).reshape(head_count, block_count, BLOCK), axis=-1)
    block_decay = cumulative[..., -1]
    weight_log = block_decay[..., None] - cumulative + log_input
    block_max = lax.optimization_barrier(jnp.max(weight_log, axis=-1))
    weighted = key_blocks.astype(jnp.float32) * jnp.exp(weight_log - block_max[..., None])[..., None]
    normalizer = lax.optimization_barrier(jnp.sum(weighted, axis=2))
    memory = halfprod('hcsk,hcsv->hckv', weighted.astype(jnp.bfloat16), value_blocks)
    return ((query_blocks, key_blocks, value_blocks, log_input, cumulative), (block_decay, block_max, memory, normalizer))

def prefix(summary, initial):
    leading = jax.tree.map(lambda tensor: jnp.moveaxis(tensor, 1, 0), summary)

    def advance(running, current):
        return (combine(running, current), running)
    final_state, before = lax.scan(advance, initial, leading)
    return (final_state, jax.tree.map(lambda tensor: jnp.moveaxis(tensor, 0, 1), before))

def block_outputs(blocked, before):
    query_blocks, key_blocks, value_blocks, log_input, cumulative = blocked
    prior_max, prior_memory, prior_normal = (before[1], before[2], before[3])
    block_len = cumulative.shape[-1]
    scale = query_blocks.shape[-1] ** (-0.5)
    causal = jnp.tril(jnp.ones((block_len, block_len), dtype=bool))
    log_decay = jnp.where(causal, cumulative[..., :, None] - cumulative[..., None, :] + log_input[..., None, :], -jnp.inf)
    log_inter = cumulative + prior_max[..., None]
    top_value = jnp.maximum(log_inter, lax.optimization_barrier(jnp.max(log_decay, axis=-1)))
    scores = halfprod('hctk,hcsk->hcts', query_blocks, key_blocks) * scale * jnp.exp(log_decay - top_value[..., None])
    carried = jnp.exp(log_inter - top_value) * scale
    query_wide = query_blocks.astype(jnp.float32)
    numerator = carried[..., None] * jnp.einsum('hctk,hckv->hctv', query_wide, prior_memory, precision=HIGHEST_PRECISION) + halfprod('hcts,hcsv->hctv', scores.astype(jnp.bfloat16), value_blocks)
    denominator = carried * jnp.einsum('hctk,hck->hct', query_wide, prior_normal, precision=HIGHEST_PRECISION) + lax.optimization_barrier(jnp.sum(scores, axis=-1))
    return numerator / jnp.maximum(jnp.abs(denominator), jnp.exp(-top_value))[..., None]

def finish(head_values, out_gate, head_gain):
    head_count, block_count, block_len, value_width = head_values.shape
    per_head = jnp.transpose(head_values, (1, 2, 0, 3)).reshape(block_count * block_len, head_count, value_width)
    per_head = per_head * lax.rsqrt(lax.optimization_barrier(jnp.mean(per_head * per_head, axis=-1, keepdims=True)) + EPSILON)
    per_head = per_head.reshape(block_count * block_len, head_count * value_width) * head_gain
    per_head = per_head * jax.nn.sigmoid(out_gate.astype(jnp.float32))
    return per_head.astype(jnp.bfloat16)

def reference(query_rows, key_rows, value_rows, in_gate, forget_gate, out_gate, head_gain, mix_weight, expert_input, routes, route_weight, gate_weight, up_weight, down_weight):
    length = query_rows.shape[0]
    head_count = in_gate.shape[0]
    key_width = query_rows.shape[1] // head_count
    value_width = value_rows.shape[1] // head_count
    query_heads = query_rows.reshape(length, head_count, key_width).transpose(1, 0, 2)
    key_heads = key_rows.reshape(length, head_count, key_width).transpose(1, 0, 2)
    value_heads = value_rows.reshape(length, head_count, value_width).transpose(1, 0, 2)

    def one_head(current):
        query_one, key_one, value_one, input_one, forget_one = current
        blocked, summary = prepare(query_one[None], key_one[None], value_one[None], input_one[None], forget_one[None])
        final_state, before = prefix(summary, identity_state(1, key_width, value_width))
        return block_outputs(blocked, before)[0]
    head_values = lax.map(one_head, (query_heads, key_heads, value_heads, in_gate, forget_gate))
    mixed_heads = finish(head_values, out_gate, head_gain)
    mixer_out = jnp.dot(mixed_heads, mix_weight, preferred_element_type=jnp.float32).astype(jnp.bfloat16)
    squares = lax.optimization_barrier(jnp.sum(jnp.square(expert_input.astype(jnp.float32)), axis=-1))
    inverse_rms = lax.rsqrt(squares / D + EPSILON)
    slot_total = N_EP * CAP

    def one_expert(running, expert):
        matched = routes == expert
        picked = jnp.any(matched, axis=1)
        row_index = jnp.nonzero(picked, size=slot_total, fill_value=0)[0].astype(jnp.int32)
        count = jnp.sum(picked.astype(jnp.int32))
        is_valid = (jnp.arange(slot_total, dtype=jnp.int32) < count).astype(jnp.float32)
        weight = lax.optimization_barrier(jnp.sum(jnp.where(matched, route_weight, 0.0), axis=1))
        chosen = expert_input[row_index]
        row_scale = inverse_rms[row_index][:, None]
        gate_value = jnp.dot(chosen, gate_weight[expert].T, preferred_element_type=jnp.float32) * row_scale
        up_value = jnp.dot(chosen, up_weight[expert].T, preferred_element_type=jnp.float32) * row_scale
        hidden = (jax.nn.silu(gate_value) * up_value).astype(jnp.bfloat16)
        expert_rows = jnp.dot(hidden, down_weight[expert], preferred_element_type=jnp.float32).astype(jnp.bfloat16)
        term = expert_rows.astype(jnp.float32) * (weight[row_index] * is_valid)[:, None]
        return (running.at[row_index].add(term), None)
    total, _ = lax.scan(one_expert, jnp.zeros((TOKENS_B, D), jnp.float32), jnp.arange(EXPERTS, dtype=jnp.int32))
    return (mixer_out, total.astype(jnp.bfloat16))
```

```python
import functools

import jax
import jax.numpy as jnp
from jax import lax
from jax.experimental import pallas as pl
from jax.experimental.pallas import tpu as pltpu
from jax.sharding import PartitionSpec as P

EPSILON = 1e-06
LOG_FLOOR = -1e30
F32 = jnp.float32
BF16 = jnp.bfloat16
GROUPS = 4
PAD = 16


def flip(index, bits):
    place = 1
    while place <= bits:
        if bits & place:
            index = index + place * (1 - 2 * ((index // place) % 2))
        place *= 2
    return index


def dot(left, right, contract=((1,), (0,))):
    return lax.dot_general(left, right, (contract, ((), ())), preferred_element_type=F32)


def kernel(
    ep,
    tp,
    head_count,
    model_width,
    x_ref,
    slot_row_ref,
    slot_col_ref,
    weight_ref,
    a_row_ref,
    a_col_ref,
    cum_col_ref,
    gain_ref,
    q_hbm,
    k_hbm,
    v_hbm,
    og_hbm,
    wg_hbm,
    wu_hbm,
    wd_hbm,
    wm_hbm,
    mix_ref,
    exp_ref,
    q_ref,
    k_ref,
    v_ref,
    og_ref,
    wg_ref,
    wu_ref,
    wd_ref,
    wm_ref,
    slots,
    tok,
    hid,
    outb,
    ret,
    hm,
    local,
    st_in,
    st_out,
    load_sem,
    disp_send,
    disp_recv,
    tok_send,
    tok_recv,
    fwd_send,
    fwd_recv,
    hid_send,
    hid_recv,
    ret_send,
    ret_recv,
    head_send,
    head_recv,
    hfwd_send,
    hfwd_recv,
    st_send,
    st_recv,
):
    me = lax.axis_index("ep")
    mine = lax.axis_index("tp")
    cap = slots.shape[0] // ep
    span = slots.shape[0] // GROUPS
    per = ep // GROUPS
    width = x_ref.shape[1]
    length = q_ref.shape[0]
    qk = q_ref.shape[1] // head_count
    vw = v_ref.shape[1] // head_count
    units = wg_ref.shape[0]
    square = tp == 4

    loads = [
        pltpu.make_async_copy(source, target, load_sem.at[at])
        for at, (source, target) in enumerate(
            [
                (k_hbm, k_ref),
                (v_hbm, v_ref),
                (q_hbm, q_ref),
                (og_hbm, og_ref),
                (wg_hbm, wg_ref),
                (wu_hbm, wu_ref),
                (wd_hbm, wd_ref),
                (wm_hbm, wm_ref),
            ]
        )
    ]
    for load in loads:
        load.start()

    barrier = pltpu.get_barrier_semaphore()
    for i in range(1, ep):
        pl.semaphore_signal(barrier, inc=1, device_id={"ep": flip(me, i)})
    for j in range(1, tp):
        pl.semaphore_signal(barrier, inc=1, device_id={"tp": flip(mine, j)})

    tokens = x_ref.shape[0]

    def pick(group, carry):
        at = group * span
        rows = at + lax.broadcasted_iota(jnp.int32, (span, tokens), 0)
        hit = (rows == slot_row_ref[0:1, :]) | (rows == slot_row_ref[1:2, :])
        chosen = dot(hit.astype(F32).astype(BF16), x_ref[...]).astype(BF16)
        slots[pl.ds(pl.multiple_of(at, span), span), :] = chosen
        return carry

    lax.fori_loop(0, GROUPS, pick, 0)
    pl.semaphore_wait(barrier, ep - 1 + tp - 1)

    def dispatch(i):
        return pltpu.make_async_remote_copy(
            slots.at[pl.ds(i * cap, cap)],
            tok.at[0, pl.ds(i * cap, cap)],
            disp_send.at[i],
            disp_recv.at[i],
            device_id={"ep": flip(me, i)},
        )

    for i in range(1, ep):
        dispatch(i).start()
    tok[0, 0:cap, :] = slots[0:cap, :]

    def spread(group, j):
        return pltpu.make_async_remote_copy(
            tok.at[0, pl.ds(group * span, span)],
            tok.at[j, pl.ds(group * span, span)],
            tok_send.at[group, j],
            tok_recv.at[group, j],
            device_id={"tp": flip(mine, j)},
        )

    half = span // 2

    def onward(group, j):
        part = pl.ds(group * span + (j - 1) * half, half)
        return pltpu.make_async_remote_copy(
            tok.at[j, part],
            tok.at[3, part],
            fwd_send.at[group, j],
            fwd_recv.at[group, j],
            device_id={"tp": flip(mine, 3 - j)},
        )

    direct = (1, 2) if square else tuple(range(1, tp))

    def send_group(group):
        for i in range(max(1, group * per), (group + 1) * per):
            dispatch(i).wait_recv()
        for j in direct:
            spread(group, j).start()

    def relay_group(group):
        if square:
            for j in (1, 2):
                spread(group, j).wait_recv()
                onward(group, j).start()

    def collect_group(group):
        if square:
            for j in (1, 2):
                onward(group, j).wait_recv()
        else:
            for j in direct:
                spread(group, j).wait_recv()

    send_group(0)

    loads[0].wait()
    loads[1].wait()

    def summarise(h, carry):
        keys = k_ref[:, pl.ds(pl.multiple_of(h * qk, qk), qk)]
        values = v_ref[:, pl.ds(pl.multiple_of(h * vw, vw), vw)]
        top = jnp.max(a_row_ref[h], axis=1, keepdims=True)
        weighted = keys.astype(F32) * jnp.exp(a_col_ref[h] - top)
        local[h, 0:qk, :] = dot(weighted.astype(BF16), values, ((0,), (0,)))
        normal = jnp.sum(weighted, axis=0, keepdims=True)
        local[h, qk : qk + 8, 0:qk] = jnp.broadcast_to(normal, (8, qk))
        decay = cum_col_ref[h, length - 1 : length, :]
        local[h, qk + 8 : qk + 16, :] = jnp.broadcast_to(top + decay, (8, vw))
        return carry

    lax.fori_loop(0, head_count, summarise, 0)
    send_group(1)

    def chain(h):
        return pltpu.make_async_remote_copy(
            st_out.at[h],
            st_in.at[h],
            st_send.at[h],
            st_recv.at[h],
            device_id={"ep": me + 1},
        )

    @pl.when(me == 0)
    def _():
        st_in[:, 0 : qk + 8, :] = jnp.zeros((head_count, qk + 8, vw), F32)
        st_in[:, qk + 8 : qk + 16, :] = jnp.full((head_count, 8, vw), LOG_FLOOR, F32)

    for h in range(head_count):

        @pl.when(me > 0)
        def _():
            chain(h).wait_recv()

        decay = cum_col_ref[h, length - 1 : length, :]
        carried_max = st_in[h, qk + 8 : qk + 9, :] + decay
        own_max = local[h, qk + 8 : qk + 9, :]
        new_max = jnp.maximum(carried_max, own_max)
        keep = jnp.exp(carried_max - new_max)
        add = jnp.exp(own_max - new_max)
        st_out[h, 0:qk, :] = keep * st_in[h, 0:qk, :] + add * local[h, 0:qk, :]
        st_out[h, qk : qk + 8, 0:qk] = (
            keep[:, 0:qk] * st_in[h, qk : qk + 8, 0:qk]
            + add[:, 0:qk] * local[h, qk : qk + 8, 0:qk]
        )
        st_out[h, qk : qk + 8, qk:vw] = jnp.zeros((8, vw - qk), F32)
        st_out[h, qk + 8 : qk + 16, :] = jnp.broadcast_to(new_max, (8, vw))

        @pl.when(me < ep - 1)
        def _():
            chain(h).start()

    relay_group(0)
    send_group(2)
    loads[2].wait()
    loads[3].wait()

    def heads(h, carry):
        columns = pl.ds(pl.multiple_of(h * vw, vw), vw)
        queries = q_ref[:, pl.ds(pl.multiple_of(h * qk, qk), qk)]
        keys = k_ref[:, pl.ds(pl.multiple_of(h * qk, qk), qk)]
        scale = qk**-0.5
        causal = lax.broadcasted_iota(jnp.int32, (length, length), 1) <= lax.broadcasted_iota(
            jnp.int32, (length, length), 0
        )
        log_in = jnp.where(causal, a_row_ref[h], -jnp.inf)
        prior_max = st_in[h, qk + 8 : qk + 9, 0:1]
        top = jnp.maximum(prior_max, jnp.max(log_in, axis=1, keepdims=True))
        scores = dot(queries, keys, ((1,), (1,))) * scale * jnp.exp(log_in - top)
        carried = jnp.exp(prior_max - top) * scale
        memory = st_in[h, 0:qk, :]
        high = memory.astype(BF16)
        low = (memory - high.astype(F32)).astype(BF16)
        numerator = carried * (dot(queries, high) + dot(queries, low)) + dot(
            scores.astype(BF16), v_ref[:, columns]
        )
        normal = st_in[h, qk : qk + 1, 0:qk]
        denominator = carried * jnp.sum(
            queries.astype(F32) * normal, axis=1, keepdims=True
        ) + jnp.sum(scores, axis=1, keepdims=True)
        floor = jnp.exp(-(cum_col_ref[h] + top))
        value = numerator / jnp.maximum(jnp.abs(denominator), floor)
        value = value * lax.rsqrt(jnp.mean(value * value, axis=1, keepdims=True) + EPSILON)
        gate = jax.nn.sigmoid(og_ref[:, columns].astype(F32))
        hm[0, :, columns] = (value * gain_ref[:, columns] * gate).astype(BF16)
        return carry

    lax.fori_loop(0, head_count, heads, 0)
    relay_group(1)
    send_group(3)

    loads[4].wait()
    loads[5].wait()

    def expand(group):
        rows = pl.ds(group * span, span)

        gate = jnp.zeros((span, units), F32)
        up = jnp.zeros((span, units), F32)
        squares = jnp.zeros((span, 1), F32)
        for j in range(tp):
            piece = tok[j, rows, :]
            columns = pl.ds(pl.multiple_of(flip(mine, j) * width, width), width)
            gate += dot(piece, wg_ref[:, columns], ((1,), (1,)))
            up += dot(piece, wu_ref[:, columns], ((1,), (1,)))
            wide = piece.astype(F32)
            squares += jnp.sum(wide * wide, axis=1, keepdims=True)
        inverse = lax.rsqrt(squares / model_width + EPSILON)
        hid[0, rows, :] = (jax.nn.silu(gate * inverse) * (up * inverse)).astype(BF16)

    def share(group, j):
        return pltpu.make_async_remote_copy(
            hid.at[0, pl.ds(group * span, span)],
            hid.at[j, pl.ds(group * span, span)],
            hid_send.at[group, j],
            hid_recv.at[group, j],
            device_id={"tp": flip(mine, j)},
        )

    for group in range(GROUPS):
        if group + 2 < GROUPS:
            relay_group(group + 2)
        collect_group(group)
        expand(group)
        for j in range(1, tp):
            share(group, j).start()

    def head_spread(j):
        return pltpu.make_async_remote_copy(
            hm.at[0], hm.at[j], head_send.at[j], head_recv.at[j], device_id={"tp": flip(mine, j)}
        )

    def head_onward(j):
        part = pl.ds((j - 1) * (length // 2), length // 2)
        return pltpu.make_async_remote_copy(
            hm.at[j, part],
            hm.at[3, part],
            hfwd_send.at[j],
            hfwd_recv.at[j],
            device_id={"tp": flip(mine, 3 - j)},
        )

    for j in direct:
        head_spread(j).start()

    def give_back(i):
        return pltpu.make_async_remote_copy(
            outb.at[pl.ds(i * cap, cap)],
            ret.at[pl.ds(i * cap, cap)],
            ret_send.at[i],
            ret_recv.at[i],
            device_id={"ep": flip(me, i)},
        )

    loads[6].wait()
    for group in range(GROUPS - 1, -1, -1):
        rows = pl.ds(group * span, span)
        for j in range(1, tp):
            share(group, j).wait_recv()
        total = jnp.zeros((span, width), F32)
        for j in range(tp):
            at = pl.ds(pl.multiple_of(flip(mine, j) * units, units), units)
            total += dot(hid[j, rows, :], wd_ref[at, :])
        outb[rows, :] = total.astype(BF16)
        for i in range(max(1, group * per), (group + 1) * per):
            give_back(i).start()
    ret[0:cap, :] = outb[0:cap, :]

    loads[7].wait()
    if square:
        for j in (1, 2):
            head_spread(j).wait_recv()
            head_onward(j).start()
    tile = length // 2

    def mix_with(blocks):
        def step(at, carry):
            rows = pl.ds(pl.multiple_of(at * tile, tile), tile)
            total = jnp.zeros((tile, width), F32)
            for j in blocks:
                inputs = pl.ds(pl.multiple_of(flip(mine, j) * width, width), width)
                total += dot(hm[j, rows, :], wm_ref[inputs, :])
            mix_ref[rows, :] = total.astype(BF16)
            return carry

        lax.fori_loop(0, 2, step, 0)

    if square:
        for j in (1, 2):
            head_onward(j).wait_recv()
    else:
        for j in direct:
            head_spread(j).wait_recv()
    mix_with(range(tp))

    for i in range(1, ep):
        give_back(i).wait_recv()
    places = lax.broadcasted_iota(jnp.int32, (tokens, slots.shape[0]), 1)
    total = jnp.zeros((tokens, width), F32)
    for route in range(weight_ref.shape[1]):
        hit = places == slot_col_ref[:, route : route + 1]
        picked = dot(hit.astype(F32).astype(BF16), ret[...])
        total += picked * weight_ref[:, route : route + 1]
    exp_ref[...] = total.astype(BF16)

    for i in range(1, ep):
        dispatch(i).wait_send()
        give_back(i).wait_send()
    for group in range(GROUPS):
        for j in direct:
            spread(group, j).wait_send()
        for j in range(1, tp):
            share(group, j).wait_send()
        if square:
            for j in (1, 2):
                onward(group, j).wait_send()
    for j in direct:
        head_spread(j).wait_send()
    if square:
        for j in (1, 2):
            head_onward(j).wait_send()
    for h in range(head_count):

        @pl.when(me < ep - 1)
        def _():
            chain(h).wait_send()


def body(
    query_rows,
    key_rows,
    value_rows,
    in_gate,
    forget_gate,
    out_gate,
    head_gain,
    mix_weight,
    expert_input,
    routes,
    route_weight,
    gate_weight,
    up_weight,
    down_weight,
):
    ep, tp = lax.axis_size("ep"), lax.axis_size("tp")
    head_count, length = in_gate.shape
    token_count, fanout = routes.shape
    width = expert_input.shape[1]
    units = gate_weight.shape[1]
    capacity = 2 * token_count * fanout // ep
    slot_count = ep * capacity
    qk = query_rows.shape[1] // head_count
    vw = value_rows.shape[1] // head_count

    earlier = jnp.tril(jnp.ones((length, length), F32))
    cumulative = jnp.einsum(
        "hs,ts->ht", jax.nn.log_sigmoid(forget_gate), earlier, precision=lax.Precision.HIGHEST
    )
    shifted = in_gate - cumulative

    me = lax.axis_index("ep")
    turned = routes ^ me
    experts = jnp.arange(ep, dtype=jnp.int32)
    named = turned[:, :, None] == experts
    any_named = jnp.any(named, axis=1)
    before = jnp.dot(
        jnp.tril(jnp.ones((token_count, token_count), BF16), -1),
        any_named.astype(BF16),
        preferred_element_type=F32,
    ).astype(jnp.int32)
    places = experts * capacity + before
    slot_col = jnp.sum(jnp.where(named, places[:, None, :], 0), axis=2)
    slot_row = slot_col.T

    vmem = pl.BlockSpec(memory_space=pltpu.VMEM)
    anywhere = pl.BlockSpec(memory_space=pl.ANY)
    dma = pltpu.SemaphoreType.DMA
    gate_local, up_local, down_local = gate_weight[0], up_weight[0], down_weight[0]
    big = (query_rows, key_rows, value_rows, out_gate, gate_local, up_local, down_local, mix_weight)
    state = (head_count, qk + PAD, vw)
    return pl.pallas_call(
        functools.partial(kernel, ep, tp, head_count, mix_weight.shape[0]),
        out_shape=(
            jax.ShapeDtypeStruct((length, width), BF16),
            jax.ShapeDtypeStruct((token_count, width), BF16),
        ),
        in_specs=[vmem] * 8 + [anywhere] * 8,
        out_specs=(vmem, vmem),
        scratch_shapes=[pltpu.VMEM(array.shape, array.dtype) for array in big]
        + [
            pltpu.VMEM((slot_count, width), BF16),
            pltpu.VMEM((tp, slot_count, width), BF16),
            pltpu.VMEM((tp, slot_count, units), BF16),
            pltpu.VMEM((slot_count, width), BF16),
            pltpu.VMEM((slot_count, width), BF16),
            pltpu.VMEM((tp, length, width), BF16),
            pltpu.VMEM(state, F32),
            pltpu.VMEM(state, F32),
            pltpu.VMEM(state, F32),
            dma((8,)),
            dma((ep,)),
            dma((ep,)),
            dma((GROUPS, tp)),
            dma((GROUPS, tp)),
            dma((GROUPS, 4)),
            dma((GROUPS, 4)),
            dma((GROUPS, tp)),
            dma((GROUPS, tp)),
            dma((ep,)),
            dma((ep,)),
            dma((tp,)),
            dma((tp,)),
            dma((4,)),
            dma((4,)),
            dma((head_count,)),
            dma((head_count,)),
        ],
        compiler_params=pltpu.CompilerParams(
            collective_id=0, has_side_effects=True, vmem_limit_bytes=64000 * 1024
        ),
    )(
        expert_input,
        slot_row,
        slot_col,
        route_weight,
        shifted[:, None, :],
        shifted[:, :, None],
        cumulative[:, :, None],
        head_gain[None, :],
        *big,
    )


def solution(mesh):
    in_specs = (
        P("ep", "tp"),
        P("ep", "tp"),
        P("ep", "tp"),
        P("tp", "ep"),
        P("tp", "ep"),
        P("ep", "tp"),
        P("tp"),
        P(None, "tp"),
        P("ep", "tp"),
        P("ep", None),
        P("ep", None),
        P("ep", "tp", None),
        P("ep", "tp", None),
        P("ep", None, "tp"),
    )
    out_specs = (P("ep", "tp"), P("ep", "tp"))
    return jax.shard_map(body, mesh=mesh, in_specs=in_specs, out_specs=out_specs, check_vma=False)
```

```python
import functools

import jax
import jax.numpy as jnp
from jax import lax
from jax.experimental import pallas as pl
from jax.experimental.pallas import tpu as pltpu
from jax.sharding import PartitionSpec as P

EPSILON = 1e-06
LOG_FLOOR = -1e30
F32 = jnp.float32
BF16 = jnp.bfloat16
GROUPS = 4
PAD = 16


def flip(index, bits):
    place = 1
    while place <= bits:
        if bits & place:
            index = index + place * (1 - 2 * ((index // place) % 2))
        place *= 2
    return index


def dot(left, right, contract=((1,), (0,))):
    return lax.dot_general(left, right, (contract, ((), ())), preferred_element_type=F32)


def upright(row):
    size = row.shape[1]
    own = lax.broadcasted_iota(jnp.int32, (size, size), 0) == lax.broadcasted_iota(
        jnp.int32, (size, size), 1
    )
    return jnp.sum(jnp.where(own, row, jnp.zeros((), row.dtype)), axis=1, keepdims=True)


def kernel(
    ep,
    tp,
    head_count,
    model_width,
    x_ref,
    slot_row_ref,
    weight_ref,
    a_ref,
    cum_ref,
    gain_ref,
    q_hbm,
    k_hbm,
    v_hbm,
    og_hbm,
    wg_hbm,
    wu_hbm,
    wd_hbm,
    wm_hbm,
    mix_ref,
    exp_ref,
    q_ref,
    k_ref,
    v_ref,
    og_ref,
    wg_ref,
    wu_ref,
    wd_ref,
    wm_ref,
    slots,
    tok,
    hid,
    outb,
    ret,
    hm,
    local,
    st_in,
    st_out,
    load_sem,
    disp_send,
    disp_recv,
    tok_send,
    tok_recv,
    fwd_send,
    fwd_recv,
    hid_send,
    hid_recv,
    ret_send,
    ret_recv,
    head_send,
    head_recv,
    hfwd_send,
    hfwd_recv,
    st_send,
    st_recv,
):
    me = lax.axis_index("ep")
    mine = lax.axis_index("tp")
    cap = slots.shape[0] // ep
    span = slots.shape[0] // GROUPS
    per = ep // GROUPS
    width = x_ref.shape[1]
    length = q_ref.shape[0]
    qk = q_ref.shape[1] // head_count
    vw = v_ref.shape[1] // head_count
    units = wg_ref.shape[0]
    square = tp == 4

    loads = [
        pltpu.make_async_copy(source, target, load_sem.at[at])
        for at, (source, target) in enumerate(
            [
                (k_hbm, k_ref),
                (v_hbm, v_ref),
                (q_hbm, q_ref),
                (og_hbm, og_ref),
                (wg_hbm, wg_ref),
                (wu_hbm, wu_ref),
                (wd_hbm, wd_ref),
                (wm_hbm, wm_ref),
            ]
        )
    ]
    for load in loads:
        load.start()

    barrier = pltpu.get_barrier_semaphore()
    for i in range(1, ep):
        pl.semaphore_signal(barrier, inc=1, device_id={"ep": flip(me, i)})
    for j in range(1, tp):
        pl.semaphore_signal(barrier, inc=1, device_id={"tp": flip(mine, j)})

    tokens = x_ref.shape[0]

    def pick(group, carry):
        at = group * span
        rows = at + lax.broadcasted_iota(jnp.int32, (span, tokens), 0)
        hit = (rows == slot_row_ref[0:1, :]) | (rows == slot_row_ref[1:2, :])
        chosen = dot(hit.astype(F32).astype(BF16), x_ref[...]).astype(BF16)
        slots[pl.ds(pl.multiple_of(at, span), span), :] = chosen
        return carry

    lax.fori_loop(0, GROUPS, pick, 0)
    pl.semaphore_wait(barrier, ep - 1 + tp - 1)

    def dispatch(i):
        return pltpu.make_async_remote_copy(
            slots.at[pl.ds(i * cap, cap)],
            tok.at[0, pl.ds(i * cap, cap)],
            disp_send.at[i],
            disp_recv.at[i],
            device_id={"ep": flip(me, i)},
        )

    near = per
    far = [i for i in range(2 * per, ep)] + [i for i in range(per, 2 * per)]
    waits_for_chain = me % 2 == 1
    for i in [i for i in range(1, per)] + far:
        if i < near:
            dispatch(i).start()
        else:
            held = waits_for_chain & (flip(me, i) > me)

            @pl.when(jnp.logical_not(held))
            def _():
                dispatch(i).start()

    tok[0, 0:cap, :] = slots[0:cap, :]

    def spread(group, j):
        return pltpu.make_async_remote_copy(
            tok.at[0, pl.ds(group * span, span)],
            tok.at[j, pl.ds(group * span, span)],
            tok_send.at[group, j],
            tok_recv.at[group, j],
            device_id={"tp": flip(mine, j)},
        )

    half = span // 2

    def onward(group, j):
        part = pl.ds(group * span + (j - 1) * half, half)
        return pltpu.make_async_remote_copy(
            tok.at[j, part],
            tok.at[3, part],
            fwd_send.at[group, j],
            fwd_recv.at[group, j],
            device_id={"tp": flip(mine, 3 - j)},
        )

    direct = (1, 2) if square else tuple(range(1, tp))

    def send_group(group):
        for i in range(max(1, group * per), (group + 1) * per):
            dispatch(i).wait_recv()
        for j in direct:
            spread(group, j).start()

    def relay_group(group):
        if square:
            for j in (1, 2):
                spread(group, j).wait_recv()
                onward(group, j).start()

    def collect_group(group):
        if square:
            for j in (1, 2):
                onward(group, j).wait_recv()
        else:
            for j in direct:
                spread(group, j).wait_recv()

    send_group(0)

    loads[0].wait()
    loads[1].wait()

    def summarise(h, carry):
        keys = k_ref[:, pl.ds(pl.multiple_of(h * qk, qk), qk)]
        values = v_ref[:, pl.ds(pl.multiple_of(h * vw, vw), vw)]
        log_in = a_ref[pl.ds(h, 1), :]
        top = jnp.max(log_in, axis=1, keepdims=True)
        weighted = keys.astype(F32) * jnp.exp(upright(log_in) - top)
        local[h, 0:qk, :] = dot(weighted.astype(BF16), values, ((0,), (0,)))
        normal = jnp.sum(weighted, axis=0, keepdims=True)
        local[h, qk : qk + 8, 0:qk] = jnp.broadcast_to(normal, (8, qk))
        decay = cum_ref[pl.ds(h, 1), :][:, length - 1 : length]
        local[h, qk + 8 : qk + 16, :] = jnp.broadcast_to(top + decay, (8, vw))
        return carry

    lax.fori_loop(0, head_count, summarise, 0)

    @pl.when(me >= ep // 2)
    def _():
        relay_group(0)

    def chain(h):
        return pltpu.make_async_remote_copy(
            st_out.at[h],
            st_in.at[h],
            st_send.at[h],
            st_recv.at[h],
            device_id={"ep": me + 1},
        )

    @pl.when(me == 0)
    def _():
        st_in[:, 0 : qk + 8, :] = jnp.zeros((head_count, qk + 8, vw), F32)
        st_in[:, qk + 8 : qk + 16, :] = jnp.full((head_count, 8, vw), LOG_FLOOR, F32)

    for h in range(head_count):

        @pl.when(me > 0)
        def _():
            chain(h).wait_recv()

        decay = cum_ref[h : h + 1, length - 1 : length]
        carried_max = st_in[h, qk + 8 : qk + 9, :] + decay
        own_max = local[h, qk + 8 : qk + 9, :]
        new_max = jnp.maximum(carried_max, own_max)
        keep = jnp.exp(carried_max - new_max)
        add = jnp.exp(own_max - new_max)
        st_out[h, 0:qk, :] = keep * st_in[h, 0:qk, :] + add * local[h, 0:qk, :]
        st_out[h, qk : qk + 8, 0:qk] = (
            keep[:, 0:qk] * st_in[h, qk : qk + 8, 0:qk]
            + add[:, 0:qk] * local[h, qk : qk + 8, 0:qk]
        )
        st_out[h, qk : qk + 8, qk:vw] = jnp.zeros((8, vw - qk), F32)
        st_out[h, qk + 8 : qk + 16, :] = jnp.broadcast_to(new_max, (8, vw))

        @pl.when(me < ep - 1)
        def _():
            chain(h).start()

    for i in far:
        held = waits_for_chain & (flip(me, i) > me)

        @pl.when(held)
        def _():
            dispatch(i).start()

    @pl.when(me < ep // 2)
    def _():
        relay_group(0)

    send_group(2)

    loads[2].wait()
    loads[3].wait()

    def heads(h, carry):
        columns = pl.ds(pl.multiple_of(h * vw, vw), vw)
        queries = q_ref[:, pl.ds(pl.multiple_of(h * qk, qk), qk)]
        keys = k_ref[:, pl.ds(pl.multiple_of(h * qk, qk), qk)]
        scale = qk**-0.5
        causal = lax.broadcasted_iota(jnp.int32, (length, length), 1) <= lax.broadcasted_iota(
            jnp.int32, (length, length), 0
        )
        log_in = jnp.where(causal, a_ref[pl.ds(h, 1), :], -jnp.inf)
        prior_max = st_in[h, qk + 8 : qk + 9, 0:1]
        top = jnp.maximum(prior_max, jnp.max(log_in, axis=1, keepdims=True))
        scores = dot(queries, keys, ((1,), (1,))) * scale * jnp.exp(log_in - top)
        carried = jnp.exp(prior_max - top) * scale
        memory = st_in[h, 0:qk, :]
        high = memory.astype(BF16)
        low = (memory - high.astype(F32)).astype(BF16)
        numerator = carried * (dot(queries, high) + dot(queries, low)) + dot(
            scores.astype(BF16), v_ref[:, columns]
        )
        normal = st_in[h, qk : qk + 1, 0:qk]
        denominator = carried * jnp.sum(
            queries.astype(F32) * normal, axis=1, keepdims=True
        ) + jnp.sum(scores, axis=1, keepdims=True)
        floor = jnp.exp(-(upright(cum_ref[pl.ds(h, 1), :]) + top))
        value = numerator / jnp.maximum(jnp.abs(denominator), floor)
        value = value * lax.rsqrt(jnp.mean(value * value, axis=1, keepdims=True) + EPSILON)
        gate = jax.nn.sigmoid(og_ref[:, columns].astype(F32))
        hm[0, :, columns] = (value * gain_ref[:, columns] * gate).astype(BF16)
        return carry

    lax.fori_loop(0, head_count, heads, 0)
    relay_group(2)

    loads[4].wait()
    loads[5].wait()

    def expand(group):
        rows = pl.ds(group * span, span)

        gate = jnp.zeros((span, units), F32)
        up = jnp.zeros((span, units), F32)
        squares = jnp.zeros((span, 1), F32)
        for j in range(tp):
            piece = tok[j, rows, :]
            columns = pl.ds(pl.multiple_of(flip(mine, j) * width, width), width)
            gate += dot(piece, wg_ref[:, columns], ((1,), (1,)))
            up += dot(piece, wu_ref[:, columns], ((1,), (1,)))
            wide = piece.astype(F32)
            squares += jnp.sum(wide * wide, axis=1, keepdims=True)
        inverse = lax.rsqrt(squares / model_width + EPSILON)
        hid[0, rows, :] = (jax.nn.silu(gate * inverse) * (up * inverse)).astype(BF16)

    def share(group, j):
        return pltpu.make_async_remote_copy(
            hid.at[0, pl.ds(group * span, span)],
            hid.at[j, pl.ds(group * span, span)],
            hid_send.at[group, j],
            hid_recv.at[group, j],
            device_id={"tp": flip(mine, j)},
        )

    def give_back(i):
        return pltpu.make_async_remote_copy(
            outb.at[pl.ds(i * cap, cap)],
            ret.at[pl.ds(i * cap, cap)],
            ret_send.at[i],
            ret_recv.at[i],
            device_id={"ep": flip(me, i)},
        )

    def contract(group):
        rows = pl.ds(group * span, span)
        for j in range(1, tp):
            share(group, j).wait_recv()
        total = jnp.zeros((span, width), F32)
        for j in range(tp):
            at = pl.ds(pl.multiple_of(flip(mine, j) * units, units), units)
            total += dot(hid[j, rows, :], wd_ref[at, :])
        outb[rows, :] = total.astype(BF16)
        for i in range(max(1, group * per), (group + 1) * per):
            give_back(i).start()

    tile = length // 2

    def head_spread(part, j):
        rows = pl.ds(part * tile, tile)
        return pltpu.make_async_remote_copy(
            hm.at[0, rows],
            hm.at[j, rows],
            head_send.at[part, j],
            head_recv.at[part, j],
            device_id={"tp": flip(mine, j)},
        )

    def head_onward(part, j):
        rows = pl.ds(part * tile + (j - 1) * (tile // 2), tile // 2)
        return pltpu.make_async_remote_copy(
            hm.at[j, rows],
            hm.at[3, rows],
            hfwd_send.at[part, j],
            hfwd_recv.at[part, j],
            device_id={"tp": flip(mine, 3 - j)},
        )

    def expand_and_share(group):
        collect_group(group)
        expand(group)
        for j in range(1, tp):
            share(group, j).start()

    def head_relay(part):
        if square:
            for j in (1, 2):
                head_spread(part, j).wait_recv()
                head_onward(part, j).start()

    def mix(part):
        rows = pl.ds(part * tile, tile)
        for j in range(1, tp):
            if not square:
                head_spread(part, j).wait_recv()
            elif j < 3:
                head_onward(part, j).wait_recv()
        total = jnp.zeros((tile, width), F32)
        for j in range(tp):
            inputs = pl.ds(pl.multiple_of(flip(mine, j) * width, width), width)
            total += dot(hm[j, rows, :], wm_ref[inputs, :])
        mix_ref[rows, :] = total.astype(BF16)

    for j in direct:
        head_spread(0, j).start()
    send_group(3)
    loads[6].wait()
    loads[7].wait()
    expand_and_share(0)
    relay_group(3)
    send_group(1)
    expand_and_share(2)
    contract(0)
    ret[0:cap, :] = outb[0:cap, :]
    relay_group(1)
    head_relay(0)
    expand_and_share(3)
    contract(2)
    expand_and_share(1)
    for j in direct:
        head_spread(1, j).start()
    contract(3)
    mix(0)
    contract(1)
    head_relay(1)

    for i in range(1, ep):
        give_back(i).wait_recv()
    places = lax.broadcasted_iota(jnp.int32, (slots.shape[0], tokens), 0)
    total = jnp.zeros((tokens, width), F32)
    for route in range(weight_ref.shape[0]):
        hit = places == slot_row_ref[route : route + 1, :]
        picked = dot(hit.astype(F32).astype(BF16), ret[...], ((0,), (0,)))
        total += picked * upright(weight_ref[route : route + 1, :])
    exp_ref[...] = total.astype(BF16)

    mix(1)

    for i in range(1, ep):
        dispatch(i).wait_send()
        give_back(i).wait_send()
    for group in range(GROUPS):
        for j in direct:
            spread(group, j).wait_send()
        for j in range(1, tp):
            share(group, j).wait_send()
        if square:
            for j in (1, 2):
                onward(group, j).wait_send()
    for part in range(2):
        for j in direct:
            head_spread(part, j).wait_send()
        if square:
            for j in (1, 2):
                head_onward(part, j).wait_send()
    for h in range(head_count):

        @pl.when(me < ep - 1)
        def _():
            chain(h).wait_send()


def body(
    query_rows,
    key_rows,
    value_rows,
    in_gate,
    forget_gate,
    out_gate,
    head_gain,
    mix_weight,
    expert_input,
    routes,
    route_weight,
    gate_weight,
    up_weight,
    down_weight,
):
    ep, tp = lax.axis_size("ep"), lax.axis_size("tp")
    head_count, length = in_gate.shape
    token_count, fanout = routes.shape
    width = expert_input.shape[1]
    units = gate_weight.shape[1]
    capacity = 2 * token_count * fanout // ep
    slot_count = ep * capacity
    qk = query_rows.shape[1] // head_count
    vw = value_rows.shape[1] // head_count

    earlier = jnp.tril(jnp.ones((length, length), F32))
    cumulative = jnp.einsum(
        "hs,ts->ht", jax.nn.log_sigmoid(forget_gate), earlier, precision=lax.Precision.HIGHEST
    )
    shifted = in_gate - cumulative

    me = lax.axis_index("ep")
    turned = routes ^ me
    experts = jnp.arange(ep, dtype=jnp.int32)
    named = turned[:, :, None] == experts
    any_named = jnp.any(named, axis=1)
    before = jnp.dot(
        jnp.tril(jnp.ones((token_count, token_count), BF16), -1),
        any_named.astype(BF16),
        preferred_element_type=F32,
    ).astype(jnp.int32)
    places = experts * capacity + before
    slot_row = jnp.sum(jnp.where(named, places[:, None, :], 0), axis=2).T

    vmem = pl.BlockSpec(memory_space=pltpu.VMEM)
    anywhere = pl.BlockSpec(memory_space=pl.ANY)
    dma = pltpu.SemaphoreType.DMA
    gate_local, up_local, down_local = gate_weight[0], up_weight[0], down_weight[0]
    big = (query_rows, key_rows, value_rows, out_gate, gate_local, up_local, down_local, mix_weight)
    state = (head_count, qk + PAD, vw)
    return pl.pallas_call(
        functools.partial(kernel, ep, tp, head_count, mix_weight.shape[0]),
        out_shape=(
            jax.ShapeDtypeStruct((length, width), BF16),
            jax.ShapeDtypeStruct((token_count, width), BF16),
        ),
        in_specs=[vmem] * 6 + [anywhere] * 8,
        out_specs=(vmem, vmem),
        scratch_shapes=[pltpu.VMEM(array.shape, array.dtype) for array in big]
        + [
            pltpu.VMEM((slot_count, width), BF16),
            pltpu.VMEM((tp, slot_count, width), BF16),
            pltpu.VMEM((tp, slot_count, units), BF16),
            pltpu.VMEM((slot_count, width), BF16),
            pltpu.VMEM((slot_count, width), BF16),
            pltpu.VMEM((tp, length, width), BF16),
            pltpu.VMEM(state, F32),
            pltpu.VMEM(state, F32),
            pltpu.VMEM(state, F32),
            dma((8,)),
            dma((ep,)),
            dma((ep,)),
            dma((GROUPS, tp)),
            dma((GROUPS, tp)),
            dma((GROUPS, 4)),
            dma((GROUPS, 4)),
            dma((GROUPS, tp)),
            dma((GROUPS, tp)),
            dma((ep,)),
            dma((ep,)),
            dma((2, tp)),
            dma((2, tp)),
            dma((2, 4)),
            dma((2, 4)),
            dma((head_count,)),
            dma((head_count,)),
        ],
        compiler_params=pltpu.CompilerParams(
            collective_id=0, has_side_effects=True, vmem_limit_bytes=64000 * 1024
        ),
    )(
        expert_input,
        slot_row,
        route_weight.T,
        shifted,
        cumulative,
        head_gain[None, :],
        *big,
    )


def solution(mesh):
    in_specs = (
        P("ep", "tp"),
        P("ep", "tp"),
        P("ep", "tp"),
        P("tp", "ep"),
        P("tp", "ep"),
        P("ep", "tp"),
        P("tp"),
        P(None, "tp"),
        P("ep", "tp"),
        P("ep", None),
        P("ep", None),
        P("ep", "tp", None),
        P("ep", "tp", None),
        P("ep", None, "tp"),
    )
    out_specs = (P("ep", "tp"), P("ep", "tp"))
    return jax.shard_map(body, mesh=mesh, in_specs=in_specs, out_specs=out_specs, check_vma=False)
```

```python
import functools

import jax
import jax.numpy as jnp
from jax import lax
from jax.experimental import pallas as pl
from jax.experimental.pallas import tpu as pltpu
from jax.sharding import PartitionSpec as P

EPSILON = 1e-06
LOG_FLOOR = -1e30
F32 = jnp.float32
BF16 = jnp.bfloat16
GROUPS = 4
PAD = 16


def flip(index, bits):
    place = 1
    while place <= bits:
        if bits & place:
            index = index + place * (1 - 2 * ((index // place) % 2))
        place *= 2
    return index


def dot(left, right, contract=((1,), (0,))):
    return lax.dot_general(left, right, (contract, ((), ())), preferred_element_type=F32)


def upright(row):
    size = row.shape[1]
    own = lax.broadcasted_iota(jnp.int32, (size, size), 0) == lax.broadcasted_iota(
        jnp.int32, (size, size), 1
    )
    return jnp.sum(jnp.where(own, row, jnp.zeros((), row.dtype)), axis=1, keepdims=True)


def kernel(
    ep,
    tp,
    head_count,
    model_width,
    x_ref,
    slot_row_ref,
    weight_ref,
    a_ref,
    cum_ref,
    gain_ref,
    q_hbm,
    k_hbm,
    v_hbm,
    og_hbm,
    wg_hbm,
    wu_hbm,
    wd_hbm,
    wm_hbm,
    mix_ref,
    exp_ref,
    q_ref,
    k_ref,
    v_ref,
    og_ref,
    wg_ref,
    wu_ref,
    wd_ref,
    wm_ref,
    slots,
    tok,
    hid,
    outb,
    ret,
    hm,
    local,
    st_in,
    st_out,
    load_sem,
    disp_send,
    disp_recv,
    tok_send,
    tok_recv,
    fwd_send,
    fwd_recv,
    hid_send,
    hid_recv,
    ret_send,
    ret_recv,
    head_send,
    head_recv,
    hfwd_send,
    hfwd_recv,
    st_send,
    st_recv,
):
    me = lax.axis_index("ep")
    mine = lax.axis_index("tp")
    cap = slots.shape[0] // ep
    span = slots.shape[0] // GROUPS
    per = ep // GROUPS
    width = x_ref.shape[1]
    length = q_ref.shape[0]
    qk = q_ref.shape[1] // head_count
    vw = v_ref.shape[1] // head_count
    units = wg_ref.shape[0]
    square = tp == 4

    loads = [
        pltpu.make_async_copy(source, target, load_sem.at[at])
        for at, (source, target) in enumerate(
            [
                (k_hbm, k_ref),
                (v_hbm, v_ref),
                (q_hbm, q_ref),
                (og_hbm, og_ref),
                (wg_hbm, wg_ref),
                (wu_hbm, wu_ref),
                (wd_hbm, wd_ref),
                (wm_hbm, wm_ref),
            ]
        )
    ]
    for load in loads:
        load.start()

    barrier = pltpu.get_barrier_semaphore()
    for i in range(1, ep):
        pl.semaphore_signal(barrier, inc=1, device_id={"ep": flip(me, i)})
    for j in range(1, tp):
        pl.semaphore_signal(barrier, inc=1, device_id={"tp": flip(mine, j)})

    tokens = x_ref.shape[0]

    def pick(group, carry):
        at = group * span
        rows = at + lax.broadcasted_iota(jnp.int32, (span, tokens), 0)
        hit = (rows == slot_row_ref[0:1, :]) | (rows == slot_row_ref[1:2, :])
        chosen = dot(hit.astype(F32).astype(BF16), x_ref[...]).astype(BF16)
        slots[pl.ds(pl.multiple_of(at, span), span), :] = chosen
        return carry

    lax.fori_loop(0, GROUPS, pick, 0)
    pl.semaphore_wait(barrier, ep - 1 + tp - 1)

    def dispatch(i):
        return pltpu.make_async_remote_copy(
            slots.at[pl.ds(i * cap, cap)],
            tok.at[0, pl.ds(i * cap, cap)],
            disp_send.at[i],
            disp_recv.at[i],
            device_id={"ep": flip(me, i)},
        )

    near = max(2, 2 * per)
    waits_for_chain = me % 2 == 1
    for i in range(1, ep):
        if i < near:
            dispatch(i).start()
        else:
            held = waits_for_chain & (flip(me, i) > me)

            @pl.when(jnp.logical_not(held))
            def _():
                dispatch(i).start()

    tok[0, 0:cap, :] = slots[0:cap, :]

    def spread(group, j):
        return pltpu.make_async_remote_copy(
            tok.at[0, pl.ds(group * span, span)],
            tok.at[j, pl.ds(group * span, span)],
            tok_send.at[group, j],
            tok_recv.at[group, j],
            device_id={"tp": flip(mine, j)},
        )

    half = span // 2

    def onward(group, j):
        part = pl.ds(group * span + (j - 1) * half, half)
        return pltpu.make_async_remote_copy(
            tok.at[j, part],
            tok.at[3, part],
            fwd_send.at[group, j],
            fwd_recv.at[group, j],
            device_id={"tp": flip(mine, 3 - j)},
        )

    direct = (1, 2) if square else tuple(range(1, tp))

    def send_group(group):
        for i in range(max(1, group * per), (group + 1) * per):
            dispatch(i).wait_recv()
        for j in direct:
            spread(group, j).start()

    def relay_group(group):
        if square:
            for j in (1, 2):
                spread(group, j).wait_recv()
                onward(group, j).start()

    def collect_group(group):
        if square:
            for j in (1, 2):
                onward(group, j).wait_recv()
        else:
            for j in direct:
                spread(group, j).wait_recv()

    send_group(0)

    loads[0].wait()
    loads[1].wait()

    def summarise(h, carry):
        keys = k_ref[:, pl.ds(pl.multiple_of(h * qk, qk), qk)]
        values = v_ref[:, pl.ds(pl.multiple_of(h * vw, vw), vw)]
        log_in = a_ref[pl.ds(h, 1), :]
        top = jnp.max(log_in, axis=1, keepdims=True)
        weighted = keys.astype(F32) * jnp.exp(upright(log_in) - top)
        local[h, 0:qk, :] = dot(weighted.astype(BF16), values, ((0,), (0,)))
        normal = jnp.sum(weighted, axis=0, keepdims=True)
        local[h, qk : qk + 8, 0:qk] = jnp.broadcast_to(normal, (8, qk))
        decay = cum_ref[pl.ds(h, 1), :][:, length - 1 : length]
        local[h, qk + 8 : qk + 16, :] = jnp.broadcast_to(top + decay, (8, vw))
        return carry

    lax.fori_loop(0, head_count, summarise, 0)

    @pl.when(me >= ep // 2)
    def _():
        send_group(1)
        relay_group(0)

    def chain(h):
        return pltpu.make_async_remote_copy(
            st_out.at[h],
            st_in.at[h],
            st_send.at[h],
            st_recv.at[h],
            device_id={"ep": me + 1},
        )

    @pl.when(me == 0)
    def _():
        st_in[:, 0 : qk + 8, :] = jnp.zeros((head_count, qk + 8, vw), F32)
        st_in[:, qk + 8 : qk + 16, :] = jnp.full((head_count, 8, vw), LOG_FLOOR, F32)

    for h in range(head_count):

        @pl.when(me > 0)
        def _():
            chain(h).wait_recv()

        decay = cum_ref[h : h + 1, length - 1 : length]
        carried_max = st_in[h, qk + 8 : qk + 9, :] + decay
        own_max = local[h, qk + 8 : qk + 9, :]
        new_max = jnp.maximum(carried_max, own_max)
        keep = jnp.exp(carried_max - new_max)
        add = jnp.exp(own_max - new_max)
        st_out[h, 0:qk, :] = keep * st_in[h, 0:qk, :] + add * local[h, 0:qk, :]
        st_out[h, qk : qk + 8, 0:qk] = (
            keep[:, 0:qk] * st_in[h, qk : qk + 8, 0:qk]
            + add[:, 0:qk] * local[h, qk : qk + 8, 0:qk]
        )
        st_out[h, qk : qk + 8, qk:vw] = jnp.zeros((8, vw - qk), F32)
        st_out[h, qk + 8 : qk + 16, :] = jnp.broadcast_to(new_max, (8, vw))

        @pl.when(me < ep - 1)
        def _():
            chain(h).start()

    for i in range(near, ep):
        held = waits_for_chain & (flip(me, i) > me)

        @pl.when(held)
        def _():
            dispatch(i).start()

    @pl.when(me < ep // 2)
    def _():
        send_group(1)
        relay_group(0)

    loads[2].wait()
    loads[3].wait()

    def heads(h, carry):
        columns = pl.ds(pl.multiple_of(h * vw, vw), vw)
        queries = q_ref[:, pl.ds(pl.multiple_of(h * qk, qk), qk)]
        keys = k_ref[:, pl.ds(pl.multiple_of(h * qk, qk), qk)]
        scale = qk**-0.5
        causal = lax.broadcasted_iota(jnp.int32, (length, length), 1) <= lax.broadcasted_iota(
            jnp.int32, (length, length), 0
        )
        log_in = jnp.where(causal, a_ref[pl.ds(h, 1), :], -jnp.inf)
        prior_max = st_in[h, qk + 8 : qk + 9, 0:1]
        top = jnp.maximum(prior_max, jnp.max(log_in, axis=1, keepdims=True))
        scores = dot(queries, keys, ((1,), (1,))) * scale * jnp.exp(log_in - top)
        carried = jnp.exp(prior_max - top) * scale
        memory = st_in[h, 0:qk, :]
        high = memory.astype(BF16)
        low = (memory - high.astype(F32)).astype(BF16)
        numerator = carried * (dot(queries, high) + dot(queries, low)) + dot(
            scores.astype(BF16), v_ref[:, columns]
        )
        normal = st_in[h, qk : qk + 1, 0:qk]
        denominator = carried * jnp.sum(
            queries.astype(F32) * normal, axis=1, keepdims=True
        ) + jnp.sum(scores, axis=1, keepdims=True)
        floor = jnp.exp(-(upright(cum_ref[pl.ds(h, 1), :]) + top))
        value = numerator / jnp.maximum(jnp.abs(denominator), floor)
        value = value * lax.rsqrt(jnp.mean(value * value, axis=1, keepdims=True) + EPSILON)
        gate = jax.nn.sigmoid(og_ref[:, columns].astype(F32))
        hm[0, :, columns] = (value * gain_ref[:, columns] * gate).astype(BF16)
        return carry

    lax.fori_loop(0, head_count // 2, heads, 0)
    relay_group(1)
    send_group(2)
    lax.fori_loop(head_count // 2, head_count, heads, 0)

    loads[4].wait()
    loads[5].wait()

    def expand(group):
        rows = pl.ds(group * span, span)

        gate = jnp.zeros((span, units), F32)
        up = jnp.zeros((span, units), F32)
        squares = jnp.zeros((span, 1), F32)
        for j in range(tp):
            piece = tok[j, rows, :]
            columns = pl.ds(pl.multiple_of(flip(mine, j) * width, width), width)
            gate += dot(piece, wg_ref[:, columns], ((1,), (1,)))
            up += dot(piece, wu_ref[:, columns], ((1,), (1,)))
            wide = piece.astype(F32)
            squares += jnp.sum(wide * wide, axis=1, keepdims=True)
        inverse = lax.rsqrt(squares / model_width + EPSILON)
        hid[0, rows, :] = (jax.nn.silu(gate * inverse) * (up * inverse)).astype(BF16)

    def share(group, j):
        return pltpu.make_async_remote_copy(
            hid.at[0, pl.ds(group * span, span)],
            hid.at[j, pl.ds(group * span, span)],
            hid_send.at[group, j],
            hid_recv.at[group, j],
            device_id={"tp": flip(mine, j)},
        )

    def give_back(i):
        return pltpu.make_async_remote_copy(
            outb.at[pl.ds(i * cap, cap)],
            ret.at[pl.ds(i * cap, cap)],
            ret_send.at[i],
            ret_recv.at[i],
            device_id={"ep": flip(me, i)},
        )

    def contract(group):
        rows = pl.ds(group * span, span)
        for j in range(1, tp):
            share(group, j).wait_recv()
        total = jnp.zeros((span, width), F32)
        for j in range(tp):
            at = pl.ds(pl.multiple_of(flip(mine, j) * units, units), units)
            total += dot(hid[j, rows, :], wd_ref[at, :])
        outb[rows, :] = total.astype(BF16)
        for i in range(max(1, group * per), (group + 1) * per):
            give_back(i).start()

    tile = length // 2

    def head_spread(part, j):
        rows = pl.ds(part * tile, tile)
        return pltpu.make_async_remote_copy(
            hm.at[0, rows],
            hm.at[j, rows],
            head_send.at[part, j],
            head_recv.at[part, j],
            device_id={"tp": flip(mine, j)},
        )

    def head_onward(part, j):
        rows = pl.ds(part * tile + (j - 1) * (tile // 2), tile // 2)
        return pltpu.make_async_remote_copy(
            hm.at[j, rows],
            hm.at[3, rows],
            hfwd_send.at[part, j],
            hfwd_recv.at[part, j],
            device_id={"tp": flip(mine, 3 - j)},
        )

    def expand_and_share(group):
        collect_group(group)
        expand(group)
        for j in range(1, tp):
            share(group, j).start()

    loads[6].wait()
    for group in range(GROUPS):
        if group > 1:
            if group + 1 < GROUPS:
                relay_group(group + 1)
        expand_and_share(group)
        if group == 0:
            for later in range(3, GROUPS):
                send_group(later)
            relay_group(2)
        elif group < GROUPS - 1:
            contract(group - 1)
    for part in range(2):
        for j in direct:
            head_spread(part, j).start()
    contract(GROUPS - 2)
    contract(GROUPS - 1)
    ret[0:cap, :] = outb[0:cap, :]

    loads[7].wait()
    if square:
        for part in range(2):
            for j in (1, 2):
                head_spread(part, j).wait_recv()
                head_onward(part, j).start()

    def mix(part):
        rows = pl.ds(part * tile, tile)
        for j in range(1, tp):
            if not square:
                head_spread(part, j).wait_recv()
            elif j < 3:
                head_onward(part, j).wait_recv()
        total = jnp.zeros((tile, width), F32)
        for j in range(tp):
            inputs = pl.ds(pl.multiple_of(flip(mine, j) * width, width), width)
            total += dot(hm[j, rows, :], wm_ref[inputs, :])
        mix_ref[rows, :] = total.astype(BF16)

    mix(0)

    for i in range(1, ep):
        give_back(i).wait_recv()
    places = lax.broadcasted_iota(jnp.int32, (slots.shape[0], tokens), 0)
    total = jnp.zeros((tokens, width), F32)
    for route in range(weight_ref.shape[0]):
        hit = places == slot_row_ref[route : route + 1, :]
        picked = dot(hit.astype(F32).astype(BF16), ret[...], ((0,), (0,)))
        total += picked * upright(weight_ref[route : route + 1, :])
    exp_ref[...] = total.astype(BF16)

    mix(1)

    for i in range(1, ep):
        dispatch(i).wait_send()
        give_back(i).wait_send()
    for group in range(GROUPS):
        for j in direct:
            spread(group, j).wait_send()
        for j in range(1, tp):
            share(group, j).wait_send()
        if square:
            for j in (1, 2):
                onward(group, j).wait_send()
    for part in range(2):
        for j in direct:
            head_spread(part, j).wait_send()
        if square:
            for j in (1, 2):
                head_onward(part, j).wait_send()
    for h in range(head_count):

        @pl.when(me < ep - 1)
        def _():
            chain(h).wait_send()


def body(
    query_rows,
    key_rows,
    value_rows,
    in_gate,
    forget_gate,
    out_gate,
    head_gain,
    mix_weight,
    expert_input,
    routes,
    route_weight,
    gate_weight,
    up_weight,
    down_weight,
):
    ep, tp = lax.axis_size("ep"), lax.axis_size("tp")
    head_count, length = in_gate.shape
    token_count, fanout = routes.shape
    width = expert_input.shape[1]
    units = gate_weight.shape[1]
    capacity = 2 * token_count * fanout // ep
    slot_count = ep * capacity
    qk = query_rows.shape[1] // head_count
    vw = value_rows.shape[1] // head_count

    earlier = jnp.tril(jnp.ones((length, length), F32))
    cumulative = jnp.einsum(
        "hs,ts->ht", jax.nn.log_sigmoid(forget_gate), earlier, precision=lax.Precision.HIGHEST
    )
    shifted = in_gate - cumulative

    me = lax.axis_index("ep")
    turned = routes ^ me
    experts = jnp.arange(ep, dtype=jnp.int32)
    named = turned[:, :, None] == experts
    any_named = jnp.any(named, axis=1)
    before = jnp.dot(
        jnp.tril(jnp.ones((token_count, token_count), BF16), -1),
        any_named.astype(BF16),
        preferred_element_type=F32,
    ).astype(jnp.int32)
    places = experts * capacity + before
    slot_row = jnp.sum(jnp.where(named, places[:, None, :], 0), axis=2).T

    vmem = pl.BlockSpec(memory_space=pltpu.VMEM)
    anywhere = pl.BlockSpec(memory_space=pl.ANY)
    dma = pltpu.SemaphoreType.DMA
    gate_local, up_local, down_local = gate_weight[0], up_weight[0], down_weight[0]
    big = (query_rows, key_rows, value_rows, out_gate, gate_local, up_local, down_local, mix_weight)
    state = (head_count, qk + PAD, vw)
    return pl.pallas_call(
        functools.partial(kernel, ep, tp, head_count, mix_weight.shape[0]),
        out_shape=(
            jax.ShapeDtypeStruct((length, width), BF16),
            jax.ShapeDtypeStruct((token_count, width), BF16),
        ),
        in_specs=[vmem] * 6 + [anywhere] * 8,
        out_specs=(vmem, vmem),
        scratch_shapes=[pltpu.VMEM(array.shape, array.dtype) for array in big]
        + [
            pltpu.VMEM((slot_count, width), BF16),
            pltpu.VMEM((tp, slot_count, width), BF16),
            pltpu.VMEM((tp, slot_count, units), BF16),
            pltpu.VMEM((slot_count, width), BF16),
            pltpu.VMEM((slot_count, width), BF16),
            pltpu.VMEM((tp, length, width), BF16),
            pltpu.VMEM(state, F32),
            pltpu.VMEM(state, F32),
            pltpu.VMEM(state, F32),
            dma((8,)),
            dma((ep,)),
            dma((ep,)),
            dma((GROUPS, tp)),
            dma((GROUPS, tp)),
            dma((GROUPS, 4)),
            dma((GROUPS, 4)),
            dma((GROUPS, tp)),
            dma((GROUPS, tp)),
            dma((ep,)),
            dma((ep,)),
            dma((2, tp)),
            dma((2, tp)),
            dma((2, 4)),
            dma((2, 4)),
            dma((head_count,)),
            dma((head_count,)),
        ],
        compiler_params=pltpu.CompilerParams(
            collective_id=0, has_side_effects=True, vmem_limit_bytes=64000 * 1024
        ),
    )(
        expert_input,
        slot_row,
        route_weight.T,
        shifted,
        cumulative,
        head_gain[None, :],
        *big,
    )


def solution(mesh):
    in_specs = (
        P("ep", "tp"),
        P("ep", "tp"),
        P("ep", "tp"),
        P("tp", "ep"),
        P("tp", "ep"),
        P("ep", "tp"),
        P("tp"),
        P(None, "tp"),
        P("ep", "tp"),
        P("ep", None),
        P("ep", None),
        P("ep", "tp", None),
        P("ep", "tp", None),
        P("ep", None, "tp"),
    )
    out_specs = (P("ep", "tp"), P("ep", "tp"))
    return jax.shard_map(body, mesh=mesh, in_specs=in_specs, out_specs=out_specs, check_vma=False)
```
